32 devices in a mesh: fs: 16 (over z, y, core), tp: 2 (over x).
Axes of the slice: x: 2, y: 2, z: 4, core: 2. Of those that a mesh axis runs over, the one named last changes fastest.
Arguments:
- prompt: bfloat16 [2048, 2048], P('fs'), may hold values from -6 to 6
- norm_gain: float32 [2048], P('fs'), may hold values from 0.1 to 1.9
- gate_train: float32 [2048, 32768], P('fs', 'tp'), may hold values from -0.125 to 0.125
- up_train: float32 [2048, 32768], P('fs', 'tp'), may hold values from -0.125 to 0.125
- down_train: float32 [2048, 32768], P('fs', 'tp'), may hold values from -0.25 to 0.25
- common_gate_train: float32 [2048, 512], P('fs', 'tp'), may hold values from -0.125 to 0.125
- common_up_train: float32 [2048, 512], P('fs', 'tp'), may hold values from -0.125 to 0.125
- common_down_train: float32 [2048, 512], P('fs', 'tp'), may hold values from -0.25 to 0.25
- route_ids: int32 [2048, 6], P('fs'), may hold values from 0 to 63, all different within a row; in each aligned block of 128 rows (0 to 127, 128 to 255, ...) at most 16 rows name the same one
- route_weights: float32 [2048, 6], P('fs'), may hold values from 0.1 to 1
Outputs:
- mixture: bfloat16 [2048, 2048], P('fs', 'tp')
- gate_serve: bfloat16 [64, 512, 2048], P('fs', 'tp')
- up_serve: bfloat16 [64, 512, 2048], P('fs', 'tp')
- down_serve: bfloat16 [64, 512, 2048], P('fs', 'tp')
- common_gate_serve: bfloat16 [512, 2048], P('tp')
- common_up_serve: bfloat16 [512, 2048], P('tp')
- common_down_serve: bfloat16 [512, 2048], P('tp')
The draws below stay inside these ranges and needn't reach their ends.
Inputs may be any that keep to these rules, and one draw needn't show every extreme that they name: `route_ids`: each row names 6 different experts. Among the rows of one index of fs no expert is named more than 16 times, and in every draw some expert is named exactly 16 times by the rows of some index.
All inputs are finite; a program needn't handle non-finite values.
Results may differ from the reference program's by a relative error of at most 0.011.
Values may be sent and summed in bfloat16 or wider, within the bound.
A program may use at most 128 MiB of HBM per device.

```python
import math
import jax
import jax.numpy as jnp
import numpy as np
from jax import lax

D = 2048
FF = 512
SFF = 512
E = 64
TOP_K = 6
TOK_DEV = 128
CAP = 16
TOKENS = 2048
N_FS = 16
N_TP = 2


def shard_levels(key, extent, pieces, smallest, top_value):
    def one(dim, parts):
        draws = jax.random.uniform(jax.random.fold_in(jax.random.fold_in(key, 6), dim), (parts,), jnp.float32, smallest / len(pieces), top_value / len(pieces))
        return jnp.repeat(jnp.exp(draws), extent[dim] // parts).reshape((-1,) + (1,) * (len(extent) - dim - 1))

    factor_of = one(*pieces[0])
    for cut in pieces[1:]:
        factor_of = factor_of * one(*cut)
    return factor_of


def deal_out(rng, own, number, rows, amount, top, bound, lean):
    order = jax.random.permutation(rng, amount)
    packed, usual = portions_of(amount, rows * top, bound, lean, True), portions_of(amount, rows * top, bound, lean, False)
    places = jnp.arange(amount)

    def named(lengths, rotation):
        used = int((lengths > 0).sum())
        fixed = max(1, used // 4)
        passed = fixed + (places - fixed + rotation * (used - fixed)) % max(1, amount - fixed)
        return jnp.zeros((amount,), jnp.int32).at[order[jnp.where(places < fixed, places, passed)]].set(jnp.asarray(lengths, jnp.int32))

    lengths = jnp.where(number % 4 == 0, named(packed, number // 4), named(usual, number - number // 4 - 1))
    mixed = jax.random.permutation(jax.random.fold_in(own, 3), amount)
    giver, receiver = mixed[0:amount // 2 * 2:2], mixed[1:amount // 2 * 2:2]
    room = jnp.minimum(lengths[giver] - 1, bound - lengths[receiver]) // 2
    room = jnp.where((giver == order[0]) | (receiver == order[0]) | (lengths[receiver] == 0), 0, jnp.maximum(room, 0))
    passed = jax.random.randint(jax.random.fold_in(own, 4), (amount // 2,), 0, 1 << 20) % (room + 1)
    lengths = lengths.at[giver].add(-passed).at[receiver].add(passed)
    items = jnp.searchsorted(jnp.cumsum(lengths), jnp.arange(rows * top), side="right").astype(jnp.int32)
    listing = items.reshape(top, rows).T
    listing = listing[jax.random.permutation(jax.random.fold_in(own, 1), rows)]
    rotation = jax.random.randint(jax.random.fold_in(own, 2), (rows, 1), 0, top)
    return jnp.take_along_axis(listing, (jnp.arange(top)[None, :] + rotation) % top, axis=1)


def portions_of(amount, total, limit, skew, full):
    portions = [(1 << 20) // math.isqrt(rank ** skew) + 1 for rank in range(1, amount + 1)]
    largest = limit if full else min(limit, max(-(-total // amount), total * portions[0] // sum(portions)))
    least = 1 if total - largest >= amount - 1 else 0
    counts, rest = [largest] + [least] * (amount - 1), total - largest - least * (amount - 1)
    while rest > 0:
        free = [i for i in range(1, amount) if counts[i] < largest] or [i for i in range(1, amount) if counts[i] < limit]
        pool, budget = sum([portions[i] for i in free]), rest
        for i in free:
            extra = min(limit - counts[i], max(1, budget * portions[i] // pool), rest)
            counts[i] = counts[i] + extra
            rest = rest - extra
    return np.array(counts)


def centred(key, shape, deviation, limit, shards=(), kind=jnp.bfloat16):
    array = deviation * jax.random.normal(key, shape, jnp.float32)
    if shards:
        array = array * shard_levels(key, shape, shards, -0.22, 0.18)
    return jnp.clip(array, -limit, limit).astype(kind)


def setup_inputs(seed: int = 0) -> dict:
    key_list = jax.random.split(jax.random.key(seed), 11)
    prompt = centred(key_list[0], (TOKENS, D), 1.0, 6.0, ((0, 16),))
    norm_gain = jnp.clip(1.0 + 0.18 * jax.random.normal(key_list[1], (D,), jnp.float32), 0.1, 1.9)
    gate_train = centred(key_list[2], (D, E * FF), D ** -0.5, 0.125, ((0, 16), (1, 2)), jnp.float32)
    up_train = centred(key_list[3], (D, E * FF), D ** -0.5, 0.125, ((0, 16), (1, 2)), jnp.float32)
    down_train = centred(key_list[4], (D, E * FF), FF ** -0.5, 0.25, ((0, 16), (1, 2)), jnp.float32)
    common_gate_train = centred(key_list[5], (D, SFF), D ** -0.5, 0.125, ((0, 16), (1, 2)), jnp.float32)
    common_up_train = centred(key_list[6], (D, SFF), D ** -0.5, 0.125, ((0, 16), (1, 2)), jnp.float32)
    common_down_train = centred(key_list[7], (D, SFF), SFF ** -0.5, 0.25, ((0, 16), (1, 2)), jnp.float32)
    route_ids_keys = jax.random.split(jax.random.fold_in(key_list[8], 1), TOKENS // TOK_DEV)
    route_ids_turns = jax.random.permutation(jax.random.fold_in(key_list[8], 3), TOKENS // TOK_DEV)
    route_ids = jax.vmap(lambda own, number: deal_out(jax.random.fold_in(key_list[8], 2), own, number, TOK_DEV, E, TOP_K, CAP, 2))(route_ids_keys, route_ids_turns).reshape((TOKENS, TOP_K))
    route_weights = jnp.clip(jnp.exp(math.log(1.0) - 2.3025851 * jax.random.uniform(key_list[9], (TOKENS, TOP_K), jnp.float32) ** shard_levels(key_list[9], (TOKENS, TOP_K), ((0, 16),), -0.2, 0.2)), 0.1, 1.0)
    return {"prompt": prompt, "norm_gain": norm_gain, "gate_train": gate_train, "up_train": up_train, "down_train": down_train, "common_gate_train": common_gate_train, "common_up_train": common_up_train, "common_down_train": common_down_train, "route_ids": route_ids, "route_weights": route_weights}


epsilon = 1e-06

def slot_table(route_ids):
    groups = route_ids.reshape(N_FS, TOK_DEV * TOP_K)
    onehot = (groups[:, :, None] == jnp.arange(E, dtype=jnp.int32)[None, None, :]).astype(jnp.int32)
    before = jnp.cumsum(onehot, axis=1) - onehot
    slot_of = lax.optimization_barrier(jnp.sum(before * onehot, axis=2)).astype(jnp.int32)
    source = jnp.arange(N_FS, dtype=jnp.int32)[:, None]
    return (groups * (N_FS * CAP) + source * CAP + slot_of).reshape(-1).astype(jnp.int32)

def rounded_sum(hidden, down_matrix):
    span = hidden.shape[1] // N_TP
    running = jnp.zeros((hidden.shape[0], down_matrix.shape[1]), jnp.float32)
    for member in range(N_TP):
        partial_value = jnp.dot(hidden[:, member * span:(member + 1) * span], down_matrix[member * span:(member + 1) * span], preferred_element_type=jnp.float32).astype(jnp.bfloat16)
        running = running + lax.optimization_barrier(partial_value).astype(jnp.float32)
    return running.astype(jnp.bfloat16)

def to_serve(matrix):
    return jnp.transpose(matrix.reshape(D, E, FF), (1, 2, 0)).astype(jnp.bfloat16)

def reference(prompt, norm_gain, gate_train, up_train, down_train, common_gate_train, common_up_train, common_down_train, route_ids, route_weights):
    gain_col = norm_gain[:, None]
    gate_serve = to_serve(gate_train * gain_col)
    up_serve = to_serve(up_train * gain_col)
    down_serve = to_serve(down_train)
    common_gate_serve = jnp.transpose(common_gate_train * gain_col).astype(jnp.bfloat16)
    common_up_serve = jnp.transpose(common_up_train * gain_col).astype(jnp.bfloat16)
    common_down_serve = jnp.transpose(common_down_train).astype(jnp.bfloat16)
    values = prompt.astype(jnp.float32)
    normed = (values * lax.rsqrt(lax.optimization_barrier(jnp.mean(values * values, axis=1, keepdims=True)) + epsilon)).astype(jnp.bfloat16)
    target = slot_table(route_ids)
    pair_rows = jnp.repeat(normed, TOP_K, axis=0)
    buffer = jnp.zeros((E * N_FS * CAP, D), jnp.bfloat16).at[target].set(pair_rows).reshape(E, N_FS * CAP, D)

    def expert(operands):
        slot_rows, gate_matrix, up_matrix, down_matrix = operands
        gate_value = jnp.dot(slot_rows, gate_matrix.T, preferred_element_type=jnp.float32)
        up_value = jnp.dot(slot_rows, up_matrix.T, preferred_element_type=jnp.float32)
        hidden = (jax.nn.silu(gate_value) * up_value).astype(jnp.bfloat16)
        return rounded_sum(hidden, down_matrix)
    outputs = lax.map(expert, (buffer, gate_serve, up_serve, down_serve))
    picked = outputs.reshape(E * N_FS * CAP, D)[target].astype(jnp.float32)
    weighted = lax.optimization_barrier(jnp.sum(picked.reshape(TOKENS, TOP_K, D) * route_weights[:, :, None], axis=1))
    common_gate = jnp.dot(normed, common_gate_serve.T, preferred_element_type=jnp.float32)
    common_up = jnp.dot(normed, common_up_serve.T, preferred_element_type=jnp.float32)
    common_hidden = (jax.nn.silu(common_gate) * common_up).astype(jnp.bfloat16)
    common_out = rounded_sum(common_hidden, common_down_serve)
    mixture = (weighted + common_out.astype(jnp.float32)).astype(jnp.bfloat16)
    return (mixture, gate_serve, up_serve, down_serve, common_gate_serve, common_up_serve, common_down_serve)
```

```python
import functools

import jax
import jax.numpy as jnp
from jax import lax
from jax.experimental import pallas as pl
from jax.experimental.pallas import tpu as pltpu
from jax.sharding import PartitionSpec as P

FF = 512
E = 64
TOP_K = 6
CAP = 16
LANES = 128

epsilon = 1e-06


def silu_product(gate_value, up_value):
    return (gate_value / (1.0 + jnp.exp(-gate_value)) * up_value).astype(jnp.bfloat16)


def arrange_kernel(tp_count, chunk, unit_block, scaled, weight_ref, gain_ref, out_ref):
    for i in range(chunk):
        for p in range(tp_count):
            first = (i * tp_count + p) * unit_block
            block = weight_ref[:, first:first + unit_block]
            if scaled:
                block = block * gain_ref[...]
            out_ref[p, 0, i] = block.T.astype(jnp.bfloat16)


def arrange(weight, gain_col, scaled, tp_count, owned, chunks, which):
    width_rows = weight.shape[0]
    unit_block = FF // tp_count
    groups = weight.shape[1] // FF // owned
    chunk = owned // chunks
    if width_rows % LANES:
        low = (weight * gain_col if scaled else weight).astype(jnp.bfloat16)
        low = low.reshape(width_rows, groups, chunks, chunk, tp_count, unit_block)[:, :, which]
        return jnp.transpose(low, (3, 1, 2, 4, 0))
    out = jax.ShapeDtypeStruct((tp_count, groups, chunk, unit_block, width_rows), jnp.bfloat16)
    size = groups * chunk * FF * width_rows
    return pl.pallas_call(
        functools.partial(arrange_kernel, tp_count, chunk, unit_block, scaled),
        grid=(groups,),
        in_specs=[
            pl.BlockSpec((width_rows, chunk * FF), lambda j: (0, j * chunks + which)),
            pl.BlockSpec((width_rows, 1), lambda j: (0, 0)),
        ],
        out_specs=pl.BlockSpec((tp_count, 1, chunk, unit_block, width_rows), lambda j: (0, j, 0, 0, 0)),
        out_shape=out,
        cost_estimate=pl.CostEstimate(flops=size, bytes_accessed=6 * size, transcendentals=0),
    )(weight, gain_col)


def cross(blocks):
    tp_count = lax.axis_size("tp")
    me = lax.axis_index("tp")
    arrived = blocks
    for shift in range(1, tp_count):
        sent = lax.dynamic_index_in_dim(blocks, lax.rem(me + shift, tp_count), 0, keepdims=True)
        got = lax.ppermute(sent, "tp", [(i, (i + shift) % tp_count) for i in range(tp_count)])
        arrived = lax.dynamic_update_slice_in_dim(arrived, got, lax.rem(me - shift + tp_count, tp_count), 0)
    return arrived


def dot_t(a, b):
    return lax.dot_general(a, b, (((1,), (1,)), ((), ())), preferred_element_type=jnp.float32)


def first_kernel(sources, width_rows, rows_ref, gate_ref, up_ref, *rest):
    gate_out, up_out, hidden_ref = rest[-3:]
    for s in range(sources):
        columns = slice(s * width_rows, (s + 1) * width_rows)
        gate_out[0, :, columns] = gate_ref[s, 0]
        up_out[0, :, columns] = up_ref[s, 0]
    rows = rows_ref[0]
    hidden_ref[0] = silu_product(dot_t(rows, gate_out[0]), dot_t(rows, up_out[0]))


def second_kernel(sources, width_rows, tp_count, hidden_ref, down_ref, *rest):
    down_out, partial_ref = rest[-2:]
    for s in range(sources):
        down_out[0, :, s * width_rows:(s + 1) * width_rows] = down_ref[s, 0]
    result = jnp.dot(hidden_ref[0], down_out[0], preferred_element_type=jnp.float32).astype(jnp.bfloat16)
    share = result.shape[1] // tp_count
    for p in range(tp_count):
        for b in range(result.shape[0] // CAP):
            partial_ref[p, b, 0] = result[b * CAP:(b + 1) * CAP, p * share:(p + 1) * share]


def joined(arrived):
    sources, chunk, unit_block, width_rows = arrived.shape
    return jnp.transpose(arrived, (1, 2, 0, 3)).reshape(chunk, unit_block, sources * width_rows)


def expert_first(rows, gate, up, before, owned, which):
    sources, chunk, unit_block, width_rows = gate.shape
    slot_rows, width = rows.shape[1], rows.shape[2]
    serve = jax.ShapeDtypeStruct((owned, unit_block, width), jnp.bfloat16)
    weight_spec = pl.BlockSpec((sources, 1, unit_block, width_rows), lambda i: (0, i, 0, 0))
    serve_spec = pl.BlockSpec((1, unit_block, width), lambda i: (which * chunk + i, 0, 0))
    size = chunk * unit_block * width
    return pl.pallas_call(
        functools.partial(first_kernel, sources, width_rows),
        grid=(chunk,),
        in_specs=[pl.BlockSpec((1, slot_rows, width), lambda i: (i, 0, 0)), weight_spec, weight_spec]
        + [pl.BlockSpec(memory_space=pl.ANY)] * len(before),
        out_specs=[serve_spec, serve_spec, pl.BlockSpec((1, slot_rows, unit_block), lambda i: (i, 0, 0))],
        out_shape=[serve, serve, jax.ShapeDtypeStruct((chunk, slot_rows, unit_block), jnp.bfloat16)],
        input_output_aliases={3 + n: n for n in range(len(before))},
        cost_estimate=pl.CostEstimate(flops=4 * size * slot_rows, bytes_accessed=10 * size, transcendentals=0),
    )(rows, gate, up, *before)


def expert_second(hidden, down, before, owned, which, tp_count):
    sources, chunk, unit_block, width_rows = down.shape
    slot_rows = hidden.shape[1]
    width = sources * width_rows
    share = width // tp_count
    blocks = slot_rows // CAP
    size = chunk * unit_block * width
    return pl.pallas_call(
        functools.partial(second_kernel, sources, width_rows, tp_count),
        grid=(chunk,),
        in_specs=[
            pl.BlockSpec((1, slot_rows, unit_block), lambda i: (i, 0, 0)),
            pl.BlockSpec((sources, 1, unit_block, width_rows), lambda i: (0, i, 0, 0)),
        ]
        + [pl.BlockSpec(memory_space=pl.ANY)] * len(before),
        out_specs=[
            pl.BlockSpec((1, unit_block, width), lambda i: (which * chunk + i, 0, 0)),
            pl.BlockSpec((tp_count, blocks, 1, CAP, share), lambda i: (0, 0, i, 0, 0)),
        ],
        out_shape=[
            jax.ShapeDtypeStruct((owned, unit_block, width), jnp.bfloat16),
            jax.ShapeDtypeStruct((tp_count, blocks, chunk, CAP, share), jnp.bfloat16),
        ],
        input_output_aliases={2 + n: n for n in range(len(before))},
        cost_estimate=pl.CostEstimate(flops=2 * size * slot_rows, bytes_accessed=6 * size, transcendentals=0),
    )(hidden, down, *before)


def summed(partials):
    return jnp.sum(partials.astype(jnp.float32), axis=0).astype(jnp.bfloat16)


def local(
    prompt,
    norm_gain,
    gate_train,
    up_train,
    down_train,
    common_gate_train,
    common_up_train,
    common_down_train,
    route_ids,
    route_weights,
):
    tp_count = lax.axis_size("tp")
    fs_count = lax.axis_size("fs")
    me_tp, me_fs = lax.axis_index("tp"), lax.axis_index("fs")
    width_rows = gate_train.shape[0]
    width = width_rows * fs_count
    share = width // tp_count
    unit_block = FF // tp_count
    owned = E // fs_count
    tiled = width_rows % LANES == 0
    chunks = 2 if owned % 2 == 0 else 1
    chunk = owned // chunks
    tokens = prompt.shape[0]
    gain_col = norm_gain[:, None]

    values = prompt.astype(jnp.float32)
    normed = (
        values * lax.rsqrt(jnp.mean(values * values, axis=1, keepdims=True) + epsilon)
    ).astype(jnp.bfloat16)
    named = route_ids[:, :, None] == jnp.arange(E, dtype=jnp.int32)
    named_rows = jnp.any(named, axis=1).astype(jnp.bfloat16)
    earlier = jnp.tril(jnp.ones((tokens, tokens), jnp.bfloat16), -1)
    count = jnp.dot(earlier, named_rows, preferred_element_type=jnp.float32)
    slot_of = jnp.sum(jnp.where(named, count[:, None, :], 0.0), axis=2)
    marks = jnp.concatenate([route_ids.astype(jnp.bfloat16), slot_of.astype(jnp.bfloat16)], axis=1)
    marks = jnp.pad(marks, ((0, 0), (0, LANES - 2 * TOP_K)))
    part = tokens // tp_count
    mine = lax.dynamic_slice_in_dim(jnp.concatenate([normed, marks], axis=1), me_tp * part, part, 0)
    all_rows = lax.all_gather(mine, ("fs", "tp"), axis=0, tiled=True)
    all_rows = all_rows.reshape(fs_count, tokens, width + LANES)
    all_marks = all_rows[:, :, width:].astype(jnp.int32)
    all_ids, all_slots = all_marks[:, :, :TOP_K], all_marks[:, :, TOP_K:2 * TOP_K]
    only_rows = all_rows[:, :, :width]

    def slot_rows_of(which):
        experts = me_fs * owned + which * chunk + jnp.arange(chunk, dtype=jnp.int32)
        slots = jnp.arange(CAP, dtype=jnp.int32)
        chosen = jnp.zeros((fs_count, chunk, CAP, tokens), jnp.bool_)
        for k in range(TOP_K):
            ids_k, slots_k = all_ids[:, None, None, :, k], all_slots[:, None, None, :, k]
            chosen |= (ids_k == experts[None, :, None, None]) & (slots_k == slots[None, None, :, None])
        picked = jnp.einsum(
            "best,btd->besd", chosen.astype(jnp.bfloat16), only_rows, preferred_element_type=jnp.float32
        ).astype(jnp.bfloat16)
        return jnp.transpose(picked, (1, 0, 2, 3)).reshape(chunk, fs_count * CAP, width)

    common_low = jnp.concatenate(
        [
            jnp.transpose(common_gate_train * gain_col),
            jnp.transpose(common_up_train * gain_col),
            jnp.transpose(common_down_train),
        ],
        axis=0,
    ).astype(jnp.bfloat16)
    common_all = lax.all_gather(common_low, "fs", axis=0, tiled=False)
    common_all = jnp.transpose(common_all, (1, 0, 2)).reshape(3, unit_block, width)
    common_gate_serve, common_up_serve, common_down_serve = common_all[0], common_all[1], common_all[2]
    common_hidden = silu_product(dot_t(normed, common_gate_serve), dot_t(normed, common_up_serve))
    common_partial = jnp.dot(
        common_hidden, common_down_serve, preferred_element_type=jnp.float32
    ).astype(jnp.bfloat16)
    common_blocks = jnp.transpose(common_partial.reshape(tokens, tp_count, share), (1, 0, 2))
    common_out = summed(cross(common_blocks)).astype(jnp.float32)

    def finish_chunk(which, partial, mixed):
        expert_out = summed(cross(partial))
        returned = lax.all_to_all(expert_out, "fs", split_axis=0, concat_axis=0, tiled=True)
        returned = returned.reshape(fs_count * chunk * CAP, share)
        place = jnp.arange(fs_count * chunk * CAP, dtype=jnp.int32)
        source, rest = place // (chunk * CAP), place % (chunk * CAP)
        expert_at = source * owned + which * chunk + rest // CAP
        slot_at = rest % CAP
        slots_here = slot_of.astype(jnp.int32)
        spread_weights = jnp.zeros((tokens, place.shape[0]), jnp.float32)
        for k in range(TOP_K):
            hit = (route_ids[:, k:k + 1] == expert_at[None, :]) & (slots_here[:, k:k + 1] == slot_at[None, :])
            spread_weights += jnp.where(hit, route_weights[:, k:k + 1], 0.0)
        left = spread_weights
        for _ in range(3):
            piece = lax.reduce_precision(left, 8, 7)
            left = left - piece
            mixed = mixed + jnp.dot(
                piece.astype(jnp.bfloat16), returned, preferred_element_type=jnp.float32
            )
        return mixed

    def spread(weight, scaled, which, ahead=()):
        crossed = cross(arrange(weight, gain_col, scaled, tp_count, owned, chunks, which))
        crossed = crossed.reshape(fs_count, chunk, unit_block, width_rows)
        if ahead:
            crossed, *ahead = lax.optimization_barrier((crossed, *ahead))
        return lax.all_to_all(crossed, "fs", split_axis=0, concat_axis=0, tiled=True), *ahead

    serves, downs, gates_list = (), (), []
    mixed = common_out
    rows_of = [slot_rows_of(which) for which in range(chunks)]
    for which in range(chunks):
        gate, = spread(gate_train, True, which)
        if which > 0:
            up, mixed, hidden = spread(up_train, True, which, (mixed, hidden))
            down, partial = spread(down_train, False, which, (partial,))
        else:
            up, = spread(up_train, True, which)
            down, = spread(down_train, False, which)
        rows = rows_of[which]
        if which > 0:
            mixed = finish_chunk(which - 1, partial, mixed)
        if tiled:
            gate_serve, up_serve, hidden = expert_first(rows, gate, up, serves, owned, which)
            serves = (gate_serve, up_serve)
            down_serve, partial = expert_second(hidden, down, downs, owned, which, tp_count)
            downs = (down_serve,)
        else:
            whole = joined(gate), joined(up), joined(down)
            gates_list.append(whole)
            hidden = silu_product(
                jnp.einsum("erd,efd->erf", rows, whole[0], preferred_element_type=jnp.float32),
                jnp.einsum("erd,efd->erf", rows, whole[1], preferred_element_type=jnp.float32),
            )
            partial = jnp.einsum(
                "erf,efd->erd", hidden, whole[2], preferred_element_type=jnp.float32
            ).astype(jnp.bfloat16)
            partial = partial.reshape(chunk, fs_count, CAP, tp_count, share)
            partial = jnp.transpose(partial, (3, 1, 0, 2, 4))
    mixed = finish_chunk(chunks - 1, partial, mixed)
    if not tiled:
        gate_serve, up_serve, down_serve = (
            jnp.concatenate([item[n] for item in gates_list], axis=0) for n in range(3)
        )
    return (
        mixed.astype(jnp.bfloat16),
        gate_serve,
        up_serve,
        down_serve,
        common_gate_serve,
        common_up_serve,
        common_down_serve,
    )


def solution(mesh):
    in_specs = (
        P("fs", None),
        P("fs"),
        P("fs", "tp"),
        P("fs", "tp"),
        P("fs", "tp"),
        P("fs", "tp"),
        P("fs", "tp"),
        P("fs", "tp"),
        P("fs", None),
        P("fs", None),
    )
    out_specs = (
        P("fs", "tp"),
        P("fs", "tp", None),
        P("fs", "tp", None),
        P("fs", "tp", None),
        P("tp", None),
        P("tp", None),
        P("tp", None),
    )
    return jax.shard_map(local, mesh=mesh, in_specs=in_specs, out_specs=out_specs, check_vma=False)
```
